32 devices in a mesh: fs: 8 (over z, x), tp: 4 (over y, core).
Axes of the slice: x: 2, y: 2, z: 4, core: 2. Of those that a mesh axis runs over, the one named last changes fastest.
Arguments:
- inputs: bfloat16 [2048, 2048], P('fs'), may hold values from -6 to 6
- cotangent: bfloat16 [2048, 2048], P('fs'), may hold values from -8 to 8
- up_weight: float32 [2048, 2944], P('fs', 'tp'), may hold values from -0.125 to 0.125
- gate_weight: float32 [2048, 2944], P('fs', 'tp'), may hold values from -0.125 to 0.125
- down_weight: float32 [2944, 2048], P('tp', 'fs'), may hold values from -0.109375 to 0.109375
- up_scale: float32 [2944], P('tp'), may hold values from 0.5 to 2
- gate_scale: float32 [2944], P('tp'), may hold values from 0.5 to 2
- down_scale: float32 [2048], replicated, may hold values from 0.5 to 2
- conv_weight: float32 [3, 2944], P(None, 'tp'), may hold values from -3.5 to 3.5
- conv_bias: float32 [2944], P('tp'), may hold values from -3 to 3
Outputs:
- grad_input: bfloat16 [2048, 2048], P('fs')
- grad_up: float32 [2048, 2944], P('fs', 'tp')
- grad_gate: float32 [2048, 2944], P('fs', 'tp')
- grad_down: float32 [2944, 2048], P('tp', 'fs')
- grad_conv: float32 [3, 2944], P(None, 'tp')
- grad_bias: float32 [2944], P('tp')
The draws below stay inside these ranges and needn't reach their ends.
All inputs are finite; a program needn't handle non-finite values.
Results may differ from the reference program's by a relative error of at most 0.018.
Values may be sent and summed in bfloat16 or wider, within the bound.
A program may use at most 64 MiB of HBM per device.

```python
import math
import jax
import jax.numpy as jnp
from jax import lax

D = 2048
FF = 2944
TAPS = 3
TOK_DEV = 256
TOKENS = 2048
N_TP = 4


def raised(values, key, source, target, blocks, factor):
    def block_of(position):
        return (jnp.arange(values.shape[position]) // (values.shape[position] // blocks)).reshape((-1,) + (1,) * (values.ndim - 1 - position))

    near = jax.random.permutation(key, blocks)[block_of(target)]
    second = (block_of(target) + blocks // 2) % blocks
    return jnp.where((block_of(source) == near) | (block_of(source) == second), factor * values, values)


def steps_of(stream_key, shape, pieces, low, top_value):
    level, own = 1.0, jax.random.fold_in(stream_key, 6)
    for position, blocks in pieces:
        draws = jnp.exp(jax.random.uniform(jax.random.fold_in(own, position), (blocks,), jnp.float32, low / len(pieces), top_value / len(pieces)))
        level = level * jnp.repeat(draws, shape[position] // blocks).reshape([-1 if axis == position else 1 for axis in range(len(shape))])
    return level


def gaussian(rng, dims, scale, bound, shards=(), dtype=jnp.bfloat16):
    loudness = steps_of(rng, dims, shards, -0.22, 0.18) if shards else 1.0
    values = jax.random.normal(rng, dims, jnp.float32) * scale * loudness
    return jnp.minimum(jnp.maximum(values, -bound), bound).astype(dtype)


def gaussian_with(stream_key, extent, spread, bound, split, heavy, kind=jnp.bfloat16):
    values = spread * jax.random.normal(stream_key, extent, jnp.float32)
    if split:
        values = values * steps_of(stream_key, extent, split, -0.22, 0.18)
    return jnp.clip(raised(values, jax.random.fold_in(stream_key, 3), *heavy), -bound, bound).astype(kind)


def setup_inputs(seed: int = 0) -> dict:
    splits = jax.random.split(jax.random.key(seed), 11)
    return {
        "inputs": gaussian(splits[0], (TOKENS, D), 1.0, 6.0, ((0, 8),)),
        "cotangent": gaussian_with(splits[1], (TOKENS, D), 1.0, 8.0, ((0, 8),), (0, 1, 8, 2.0)),
        "up_weight": gaussian(splits[2], (D, FF), D ** -0.5, 0.125, ((0, 8), (1, 4)), jnp.float32),
        "gate_weight": gaussian(splits[3], (D, FF), D ** -0.5, 0.125, ((0, 8), (1, 4)), jnp.float32),
        "down_weight": gaussian(splits[4], (FF, D), FF ** -0.5, 0.109375, ((0, 4), (1, 8)), jnp.float32),
        "up_scale": jnp.clip(jnp.exp(math.log(2.0) - 1.3862944 * jax.random.uniform(splits[5], (FF,), jnp.float32) ** steps_of(splits[5], (FF,), ((0, 4),), -0.2, 0.2)), 0.5, 2.0),
        "gate_scale": jnp.clip(jnp.exp(math.log(2.0) - 1.3862944 * jax.random.uniform(splits[6], (FF,), jnp.float32) ** steps_of(splits[6], (FF,), ((0, 4),), -0.2, 0.2)), 0.5, 2.0),
        "down_scale": jnp.clip(jnp.exp(jax.random.uniform(splits[7], (D,), jnp.float32, math.log(0.5), math.log(2.0))), 0.5, 2.0),
        "conv_weight": gaussian(splits[8], (TAPS, FF), TAPS ** -0.5, 3.5, ((1, 4),), jnp.float32),
        "conv_bias": gaussian(splits[9], (FF,), 0.5, 3.0, ((0, 4),), jnp.float32),
    }


def causal_conv(act, conv_weight, conv_bias):
    seq_view = act.reshape(-1, TOK_DEV, act.shape[-1])
    padded = jnp.pad(seq_view, ((0, 0), (TAPS - 1, 0), (0, 0)))
    result = conv_bias + jnp.zeros_like(seq_view)
    for offset in range(TAPS):
        result = result + padded[:, offset:offset + TOK_DEV] * conv_weight[offset]
    return (result.reshape(act.shape), padded)

def conv_back(conv_cot, padded, conv_weight):
    seq_cot = conv_cot.reshape(-1, TOK_DEV, conv_cot.shape[-1])
    padded_cot = jnp.pad(seq_cot, ((0, 0), (0, TAPS - 1), (0, 0)))
    act_cot = jnp.zeros_like(seq_cot)
    tap_grads = []
    for offset in range(TAPS):
        shift_start = TAPS - 1 - offset
        act_cot = act_cot + conv_weight[offset] * padded_cot[:, shift_start:shift_start + TOK_DEV]
        tap_grads.append(lax.optimization_barrier(jnp.sum(seq_cot * padded[:, offset:offset + TOK_DEV], axis=(0, 1))))
    return (act_cot.reshape(conv_cot.shape), jnp.stack(tap_grads), lax.optimization_barrier(jnp.sum(seq_cot, axis=(0, 1))))

def reference(inputs, cotangent, up_weight, gate_weight, down_weight, up_scale, gate_scale, down_scale, conv_weight, conv_bias):
    up_half = up_weight.astype(jnp.bfloat16)
    gate_half = gate_weight.astype(jnp.bfloat16)
    down_half = down_weight.astype(jnp.bfloat16)
    up_act = jnp.dot(inputs, up_half, preferred_element_type=jnp.float32) * up_scale
    gate_act = jnp.dot(inputs, gate_half, preferred_element_type=jnp.float32) * gate_scale
    conv_out, padded = causal_conv(up_act, conv_weight, conv_bias)
    gelu_val, gelu_back = jax.vjp(jax.nn.gelu, conv_out)
    hidden = (gelu_val * gate_act).astype(jnp.bfloat16)
    scaled_cot = (cotangent.astype(jnp.float32) * down_scale).astype(jnp.bfloat16)
    hidden_cot = lax.dot_general(scaled_cot, down_half, (((1,), (1,)), ((), ())), preferred_element_type=jnp.float32)
    gate_cot = (hidden_cot * gelu_val * gate_scale).astype(jnp.bfloat16)
    conv_cot, = gelu_back(hidden_cot * gate_act)
    act_cot, grad_conv, grad_bias = conv_back(conv_cot, padded, conv_weight)
    up_cot = (act_cot * up_scale).astype(jnp.bfloat16)
    width = FF // N_TP
    total = jnp.zeros(inputs.shape, jnp.float32)
    for block_index in range(N_TP):
        start = block_index * width
        part = lax.dot_general(up_cot[:, start:start + width], up_half[:, start:start + width], (((1,), (1,)), ((), ())), preferred_element_type=jnp.float32)
        part = part + lax.dot_general(gate_cot[:, start:start + width], gate_half[:, start:start + width], (((1,), (1,)), ((), ())), preferred_element_type=jnp.float32)
        total = total + lax.optimization_barrier(part.astype(jnp.bfloat16)).astype(jnp.float32)
    grad_input = total.astype(jnp.bfloat16)
    grad_up = lax.dot_general(inputs, up_cot, (((0,), (0,)), ((), ())), preferred_element_type=jnp.float32)
    grad_gate = lax.dot_general(inputs, gate_cot, (((0,), (0,)), ((), ())), preferred_element_type=jnp.float32)
    grad_down = lax.dot_general(hidden, scaled_cot, (((0,), (0,)), ((), ())), preferred_element_type=jnp.float32)
    return (grad_input, grad_up, grad_gate, grad_down, grad_conv, grad_bias)
```

```python
import functools

import jax
import jax.numpy as jnp
from jax import lax
from jax.experimental import pallas as pl
from jax.experimental.pallas import tpu as pltpu
from jax.sharding import PartitionSpec as P

TAPS = 3
QUADS = 4
MESH = pl.DeviceIdType.MESH


def causal_conv(act, conv_weight, conv_bias):
    length = act.shape[1]
    padded = jnp.pad(act, ((0, 0), (TAPS - 1, 0), (0, 0)))
    result = conv_bias + jnp.zeros_like(act)
    for offset in range(TAPS):
        result = result + padded[:, offset : offset + length] * conv_weight[offset]
    return (result, padded)


def conv_back(conv_cot, padded, conv_weight):
    length = conv_cot.shape[1]
    padded_cot = jnp.pad(conv_cot, ((0, 0), (0, TAPS - 1), (0, 0)))
    act_cot = jnp.zeros_like(conv_cot)
    tap_grads = []
    for offset in range(TAPS):
        shift_start = TAPS - 1 - offset
        act_cot = act_cot + conv_weight[offset] * padded_cot[:, shift_start : shift_start + length]
        tap_grads.append(jnp.sum(conv_cot * padded[:, offset : offset + length], axis=(0, 1)))
    return (act_cot, jnp.stack(tap_grads), jnp.sum(conv_cot, axis=(0, 1)))


def contract_last(left, right):
    return lax.dot_general(
        left, right, (((1,), (1,)), ((), ())), preferred_element_type=jnp.float32
    )


def contract_first(left, right):
    return lax.dot_general(
        left, right, (((0,), (0,)), ((), ())), preferred_element_type=jnp.float32
    )


def place(n):
    wide = n // QUADS
    me, tp = lax.axis_index("fs"), lax.axis_index("tp")
    return me // wide, lax.rem(me, wide), tp, lax.rem(tp, 4)


def flip(j, bit):
    return j + bit - 2 * bit * lax.rem(j // bit, 2)


def remote(src, dst, send, recv, fs, tp):
    return pltpu.make_async_remote_copy(
        src_ref=src, dst_ref=dst, send_sem=send, recv_sem=recv,
        device_id=(fs, tp), device_id_type=MESH,
    )


def quarter(width, j):
    return pl.ds(pl.multiple_of((lax.rem(j, 2) * 2 + j // 2) * width, width), width)


def gather_kernel(n, tok, wsrc, tok_all, wall, tz_s, tz_r, tt_s, tt_r, wz_s, wz_r, wx_s, wx_r, own_s):
    wide = n // QUADS
    q, p, tp, j = place(n)
    width = tok.shape[-1] // 4
    base = tp - j
    core, side = base + flip(j, 1), base + flip(j, 2)

    barrier = pltpu.get_barrier_semaphore()
    peers = [(lax.rem(q + d, QUADS) * wide + p, tp) for d in range(1, QUADS)]
    peers += [(q * wide + lax.rem(p + d, wide), tp) for d in range(1, wide)]
    peers += [(q * wide + p, core), (q * wide + p, side)]
    for peer in peers:
        pl.semaphore_signal(barrier, inc=1, device_id=peer, device_id_type=MESH)
    pl.semaphore_wait(barrier, len(peers))

    here = q * wide + p

    def tok_z(src, s, dst_q, way):
        return remote(src, tok_all.at[:, s, :, quarter(width, j)],
                      tz_s.at[s, way], tz_r.at[s], dst_q * wide + p, tp)

    def tok_t(s, place_j, kind, dst):
        cols = quarter(width, place_j)
        return remote(tok_all.at[:, s, :, cols], tok_all.at[:, s, :, cols],
                      tt_s.at[s, kind], tt_r.at[s, place_j], here, dst)

    def w_z(src_q, dst_q):
        return remote(wsrc.at[dst_q], wall.at[src_q * wide + p],
                      wz_s.at[dst_q], wz_r.at[src_q], dst_q * wide + p, tp)

    def w_x(src, s, src_p, dst_p):
        return remote(src, wall.at[s * wide + src_p],
                      wx_s.at[s, dst_p], wx_r.at[s, src_p], q * wide + dst_p, tp)

    started = []

    def go(live, copy):
        @pl.when(live)
        def _():
            copy.start()

        started.append((live, copy))

    always = q >= 0
    own_cols = tok.at[:, :, quarter(width, j)]

    def towards(d, way):
        to = q + d if way == 0 else q - d
        live = to < QUADS if way == 0 else to >= 0
        return lax.rem(to + QUADS, QUADS), live

    def send_weights(d):
        for way in range(2):
            to, live = towards(d, way)
            go(live, w_z(q, to))

    def pass_tokens(d):
        for way in range(2):
            s, there = towards(d, 1 - way)
            onward, more = towards(1, way)
            block = tok_all.at[:, s, :, quarter(width, j)]

            @pl.when(there)
            def _():
                tok_z(own_cols, s, q, 0).wait_recv()

            go(there & more, tok_z(block, s, onward, way))
            go(there, tok_t(s, j, 0, side))
            go(there, tok_t(s, j, 1, core))

    def pass_side(d):
        for way in range(2):
            s, there = towards(d, way)

            @pl.when(there)
            def _():
                tok_t(s, flip(j, 2), 0, side).wait_recv()

            go(there, tok_t(s, flip(j, 2), 2, core))

    def pass_weights(d):
        for way in range(2):
            s, there = towards(d, way)

            @pl.when(there)
            def _():
                w_z(s, q).wait_recv()

            for e in range(1, wide):
                go(there, w_x(wall.at[s * wide + p], s, p, lax.rem(p + e, wide)))

    for way in range(2):
        to, live = towards(1, way)
        go(live, tok_z(own_cols, q, to, way))
    for d in range(1, wide):
        go(always, w_x(wsrc.at[q], q, p, lax.rem(p + d, wide)))
    send_weights(1)
    own_t = pltpu.make_async_copy(tok, tok_all.at[:, q], own_s.at[0])
    own_w = pltpu.make_async_copy(wsrc.at[q], wall.at[q * wide + p], own_s.at[1])
    own_t.start()
    own_w.start()
    pass_tokens(1)
    send_weights(2)
    pass_weights(1)
    pass_tokens(2)
    send_weights(3)
    pass_side(1)
    pass_weights(2)
    pass_tokens(3)
    pass_side(2)
    pass_side(3)
    pass_weights(3)
    for d in range(1, QUADS):
        s = lax.rem(q + d, QUADS)
        tok_t(s, flip(j, 1), 0, core).wait_recv()
        tok_t(s, flip(flip(j, 1), 2), 0, core).wait_recv()
    for s in range(QUADS):
        for e in range(1, wide):
            w_x(wsrc.at[0], s, lax.rem(p + e, wide), p).wait_recv()
    own_t.wait()
    own_w.wait()
    for live, copy in started:
        @pl.when(live)
        def _():
            copy.wait_send()


def scatter_kernel(
    n, gw, gi, small, wout, gout, smalls,
    rx, sw, rc, s1, ry, s2, rg, s3,
    x_s, x_r, z_s, z_r, c_s, c_r, y_s, y_r, g_s, g_r, t_s, t_r, m_s, m_r, own_s,
):
    wide = n // QUADS
    q, p, tp, j = place(n)
    rows = gi.shape[1]
    width = gi.shape[-1] // 4
    base = tp - j
    core, side = base + flip(j, 1), base + flip(j, 2)
    here = q * wide + p
    bit, half = lax.rem(j, 2), j // 2

    barrier = pltpu.get_barrier_semaphore()
    peers = [(lax.rem(here + d, n), tp) for d in range(1, n)]
    peers += [(here, core), (here, side)]
    for peer in peers:
        pl.semaphore_signal(barrier, inc=1, device_id=peer, device_id_type=MESH)
    pl.semaphore_wait(barrier, len(peers))

    started = []

    def go(copy):
        copy.start()
        started.append(copy)

    def at(d):
        return lax.rem(q + d, QUADS)

    def halves(b):
        return pl.ds(pl.multiple_of(b * 2 * width, 2 * width), 2 * width)

    def inner(h):
        return pl.ds(pl.multiple_of(h * width, width), width)

    def c_copy(t):
        return remote(gi.at[t, :, halves(1 - bit)], rc.at[t], c_s.at[t], c_r.at[t], here, core)

    def y_copy(t):
        return remote(s1.at[t, :, inner(1 - half)], ry.at[t], y_s.at[t], y_r.at[t], here, side)

    def g_copy(src_q, t):
        return remote(s2.at[t], rg.at[src_q], g_s.at[t], g_r.at[src_q], t * wide + p, tp)

    def x_copy(src_p, t, dst_p):
        return remote(gw.at[t * wide + dst_p], rx.at[src_p, t], x_s.at[t, dst_p], x_r.at[t, src_p],
                      q * wide + dst_p, tp)

    def z_copy(src_q, t):
        return remote(sw.at[t], wout.at[src_q], z_s.at[t], z_r.at[src_q], t * wide + p, tp)

    def m_copy(src, d):
        return remote(small, smalls.at[src], m_s.at[d], m_r.at[src], d, tp)

    def t_copy(src, place_j, kind, dst):
        return remote(src, gout.at[:, quarter(width, place_j)], t_s.at[kind], t_r.at[place_j], here, dst)

    order = [2, 1, 3, 0]
    for d in order:
        go(c_copy(at(d)))
    for d in order:
        for e in range(1, wide):
            go(x_copy(p, at(d), lax.rem(p + e, wide)))
    for d in range(1, n):
        go(m_copy(here, lax.rem(here + d, n)))
    own_m = pltpu.make_async_copy(small, smalls.at[here], own_s.at[0])
    own_m.start()

    tile = 32 if rows % 32 == 0 else rows

    def rowwise(total, body):
        step = tile if total % tile == 0 else total
        lax.fori_loop(0, total // step, lambda i, c: (body(pl.ds(pl.multiple_of(i * step, step), step)), c)[1], 0)

    def f32(v):
        return v.astype(jnp.float32)

    for d in order:
        t = at(d)
        c_copy(t).wait_recv()

        def add1(r, t=t):
            s1[t, r, :] = (f32(gi[t, r, halves(bit)]) + f32(rc[t, r, :])).astype(s1.dtype)

        rowwise(rows, add1)
        go(y_copy(t))
    for d in order:
        t = at(d)
        for e in range(1, wide):
            x_copy(lax.rem(p + e, wide), t, p).wait_recv()
        for k in range(gw.shape[1]):
            total = f32(gw[t * wide + p, k])
            for e in range(1, wide):
                total = total + f32(rx[lax.rem(p + e, wide), t, k])
            sw[t, k] = total.astype(sw.dtype)
        if d:
            go(z_copy(q, t))
        y_copy(t).wait_recv()

        def add2(r, t=t):
            s2[t, r, :] = (f32(s1[t, r, inner(half)]) + f32(ry[t, r, :])).astype(s2.dtype)

        rowwise(rows, add2)
        if d:
            go(g_copy(q, t))
    own_w = pltpu.make_async_copy(sw.at[q], wout.at[q], own_s.at[1])
    own_w.start()
    for d in range(1, QUADS):
        g_copy(at(d), q).wait_recv()

    def add3(r):
        total = f32(s2[q, r, :])
        for d in range(1, QUADS):
            total = total + f32(rg[at(d), r, :])
        s3[r, :] = total.astype(s3.dtype)

    rowwise(rows, add3)
    go(t_copy(s3, j, 0, side))
    go(t_copy(s3, j, 1, core))
    own_g = pltpu.make_async_copy(s3, gout.at[:, quarter(width, j)], own_s.at[2])
    own_g.start()
    t_copy(s3, flip(j, 2), 0, side).wait_recv()
    go(t_copy(gout.at[:, quarter(width, flip(j, 2))], flip(j, 2), 2, core))
    t_copy(s3, flip(j, 1), 0, core).wait_recv()
    t_copy(s3, flip(flip(j, 1), 2), 0, core).wait_recv()
    for d in range(1, QUADS):
        z_copy(at(d), q).wait_recv()
    for d in range(1, n):
        m_copy(lax.rem(here + d, n), here).wait_recv()
    own_m.wait()
    own_w.wait()
    own_g.wait()
    for copy in started:
        copy.wait_send()


VM = pl.BlockSpec(memory_space=pltpu.VMEM)
DMA = pltpu.SemaphoreType.DMA
BF = jnp.bfloat16


def general(
    n, n_tp,
    inputs,
    cotangent,
    up_weight,
    gate_weight,
    down_weight,
    up_scale,
    gate_scale,
    down_scale,
    conv_weight,
    conv_bias,
):
    wide = n // QUADS
    rows, cols = up_weight.shape
    part = cols // QUADS
    tokens, model = inputs.shape
    q = lax.axis_index("fs") // wide

    scaled = (cotangent.astype(jnp.float32) * down_scale).astype(BF)
    tok = jnp.stack([inputs, scaled])
    wsrc = jnp.stack([up_weight.T.astype(BF), gate_weight.T.astype(BF), down_weight.astype(BF)])
    wsrc = wsrc.reshape(3, QUADS, part, rows).transpose(1, 0, 2, 3)

    tok_all, wall = pl.pallas_call(
        functools.partial(gather_kernel, n),
        out_shape=(
            jax.ShapeDtypeStruct((2, QUADS, tokens, model), BF),
            jax.ShapeDtypeStruct((n, 3, part, rows), BF),
        ),
        in_specs=[VM] * 2,
        out_specs=(VM, VM),
        scratch_shapes=[
            DMA((QUADS, 2)), DMA((QUADS,)), DMA((QUADS, 3)), DMA((QUADS, 4)),
            DMA((QUADS,)), DMA((QUADS,)), DMA((QUADS, wide)), DMA((QUADS, wide)), DMA((2,)),
        ],
        compiler_params=pltpu.CompilerParams(
            collective_id=0, has_side_effects=True, vmem_limit_bytes=48 * 2**20
        ),
    )(tok, wsrc)

    full = wall.transpose(1, 2, 0, 3).reshape(3, part, model)
    inp = tok_all[0].reshape(QUADS * tokens, model)
    cot = tok_all[1].reshape(QUADS * tokens, model)

    def mine(v):
        return lax.dynamic_slice_in_dim(v, q * part, part, axis=v.ndim - 1)

    up_s, gate_s, taps, bias = mine(up_scale), mine(gate_scale), mine(conv_weight), mine(conv_bias)
    seq = (QUADS, tokens, part)
    up_act = (contract_last(inp, full[0]) * up_s).reshape(seq)
    gate_act = (contract_last(inp, full[1]) * gate_s).reshape(seq)
    conv_out, padded = causal_conv(up_act, taps, bias)
    gelu_val, gelu_back = jax.vjp(jax.nn.gelu, conv_out)
    hidden = (gelu_val * gate_act).astype(BF).reshape(-1, part)
    hidden_cot = contract_last(cot, full[2]).reshape(seq)
    gate_cot = (hidden_cot * gelu_val * gate_s).astype(BF).reshape(-1, part)
    (conv_cot,) = gelu_back(hidden_cot * gate_act)
    act_cot, tap_part, bias_part = conv_back(conv_cot, padded, taps)
    up_cot = (act_cot * up_s).astype(BF).reshape(-1, part)
    small = jnp.concatenate([tap_part, bias_part[None]], axis=0)
    gi = (jnp.dot(up_cot, full[0], preferred_element_type=jnp.float32)
          + jnp.dot(gate_cot, full[1], preferred_element_type=jnp.float32))
    gi = gi.astype(BF).reshape(QUADS, tokens, model)
    gw = jnp.stack([
        contract_first(up_cot, inp).astype(BF),
        contract_first(gate_cot, inp).astype(BF),
        contract_first(hidden, cot).astype(BF),
    ])
    gw = gw.reshape(3, part, n, rows).transpose(2, 0, 1, 3)

    width = model // 4
    wout, gout, smalls = pl.pallas_call(
        functools.partial(scatter_kernel, n),
        out_shape=(
            jax.ShapeDtypeStruct((QUADS, 3, part, rows), BF),
            jax.ShapeDtypeStruct((tokens, model), BF),
            jax.ShapeDtypeStruct((n,) + small.shape, jnp.float32),
        ),
        in_specs=[VM] * 3,
        out_specs=(VM, VM, VM),
        scratch_shapes=[
            pltpu.VMEM((wide, QUADS, 3, part, rows), BF),
            pltpu.VMEM((QUADS, 3, part, rows), BF),
            pltpu.VMEM((QUADS, tokens, 2 * width), BF),
            pltpu.VMEM((QUADS, tokens, 2 * width), BF),
            pltpu.VMEM((QUADS, tokens, width), BF),
            pltpu.VMEM((QUADS, tokens, width), BF),
            pltpu.VMEM((QUADS, tokens, width), BF),
            pltpu.VMEM((tokens, width), BF),
            DMA((QUADS, wide)), DMA((QUADS, wide)), DMA((QUADS,)), DMA((QUADS,)),
            DMA((QUADS,)), DMA((QUADS,)), DMA((QUADS,)), DMA((QUADS,)),
            DMA((QUADS,)), DMA((QUADS,)), DMA((3,)), DMA((4,)),
            DMA((n,)), DMA((n,)), DMA((3,)),
        ],
        compiler_params=pltpu.CompilerParams(
            collective_id=1, has_side_effects=True, vmem_limit_bytes=56 * 2**20
        ),
    )(gw, gi, small)

    if n_tp > 4:
        groups = [[g * 4 + k for g in range(n_tp // 4)] for k in range(4)]
        gout = lax.psum(gout, "tp", axis_index_groups=groups)
    stats = jnp.sum(smalls.reshape(QUADS, wide, TAPS + 1, part), axis=1)
    stats = stats.transpose(1, 0, 2).reshape(TAPS + 1, cols)
    grads = wout.transpose(1, 0, 2, 3).reshape(3, cols, rows).astype(jnp.float32)
    return (gout, grads[0].T, grads[1].T, grads[2], stats[:TAPS], stats[TAPS])


LANES = 128
CHUNKS = 2
BLOCK = 512
ROOT_2_PI = 0.7978845608028654
CUBIC = 0.044715


def follow(q):
    near = flip(q, 1)
    far = jnp.where(q < 2, 2, 1)
    last = jnp.where(q < 2, 3, 0)
    return [q, near, far, last]


def fused_kernel(
    n, inp, cot, dscale, wsrc, par, wout, gout, smalls,
    tok, wall, ct, gi, acc, gw, rx, sw, rc, s1, ry, s2, rz, s3, sm, small,
    tz_s, tz_r, tt_s, tt_r, wz_s, wz_r, wx_s, wx_r,
    c_s, c_r, y_s, y_r, g_s, g_r, t_s, t_r, x_s, x_r, z_s, z_r, m_s, m_r, own_s,
):
    wide = n // QUADS
    q, p, tp, j = place(n)
    tokens, model = inp.shape
    rows = wsrc.shape[-1]
    deep = ct.shape[1]
    width = model // 4
    base = tp - j
    core, side = base + flip(j, 1), base + flip(j, 2)
    here = q * wide + p
    bit, half = lax.rem(j, 2), j // 2
    last = QUADS - 1
    seqs = follow(q)
    always = q >= 0
    pieces = 2 * CHUNKS
    span = tokens // CHUNKS

    started = []

    def go(live, copy):
        if live is always:
            copy.start()
        else:
            @pl.when(live)
            def _():
                copy.start()

        started.append((live, copy))

    def f32(v):
        return v.astype(jnp.float32)

    def halves(b):
        return pl.ds(pl.multiple_of(b * 2 * width, 2 * width), 2 * width)

    def inner(h):
        return pl.ds(pl.multiple_of(h * width, width), width)

    def owned(fs):
        return pl.ds(pl.multiple_of(fs * rows, rows), rows)

    def piece(s, k, place_j):
        return tok.at[k // CHUNKS, s, pl.ds(k % CHUNKS * span, span), quarter(width, place_j)]

    def tok_z(s, k, way, dst_q):
        return remote(piece(s, k, j), piece(s, k, j), tz_s.at[s, way, k], tz_r.at[s, k], dst_q * wide + p, tp)

    def tok_t(s, k, place_j, kind, dst):
        ref = piece(s, k, place_j)
        return remote(ref, ref, tt_s.at[s, kind, k], tt_r.at[s, place_j, k], here, dst)

    def w_z(src_q, dst_q):
        return remote(wsrc.at[dst_q], wall.at[:, :, owned(src_q * wide + p)],
                      wz_s.at[dst_q], wz_r.at[src_q], dst_q * wide + p, tp)

    def w_x(src, s, src_p, dst_p):
        return remote(src, wall.at[:, :, owned(s * wide + src_p)],
                      wx_s.at[s, dst_p], wx_r.at[s, src_p], q * wide + dst_p, tp)

    def c_copy(t):
        return remote(gi.at[t, :, halves(1 - bit)], rc.at[t], c_s.at[t], c_r.at[t], here, core)

    def y_copy(t):
        return remote(s1.at[t, :, inner(1 - half)], ry.at[t], y_s.at[t], y_r.at[t], here, side)

    def g_copy(t, slot, dst_q):
        return remote(s2.at[t], rz.at[slot], g_s.at[t], g_r.at[slot], dst_q * wide + p, tp)

    def x_copy(src_p, t, dst_p):
        return remote(gw.at[:, :, owned(t * wide + dst_p)], rx.at[src_p, t],
                      x_s.at[t, dst_p], x_r.at[t, src_p], q * wide + dst_p, tp)

    def z_copy(src_q, t):
        return remote(sw.at[t], wout.at[src_q], z_s.at[t], z_r.at[src_q], t * wide + p, tp)

    def m_copy(src, d):
        return remote(small, smalls.at[src], m_s.at[d], m_r.at[src], d, tp)

    def t_copy(src, place_j, kind, dst):
        return remote(src, gout.at[:, quarter(width, place_j)], t_s.at[kind], t_r.at[place_j], here, dst)

    tile = 32 if tokens % 32 == 0 else tokens

    def rowwise(total, body):
        lax.fori_loop(0, total // tile, lambda i, c: (body(pl.ds(pl.multiple_of(i * tile, tile), tile)), c)[1], 0)

    barrier = pltpu.get_barrier_semaphore()
    peers = [(lax.rem(here + d, n), tp) for d in range(1, n)]
    peers += [(here, core), (here, side)]
    for peer in peers:
        pl.semaphore_signal(barrier, inc=1, device_id=peer, device_id_type=MESH)

    def prepare(r):
        tok[0, q, r, :] = inp[r, :]
        tok[1, q, r, :] = (f32(cot[r, :]) * dscale[...]).astype(tok.dtype)

    rowwise(tokens, prepare)
    sm[...] = jnp.zeros_like(sm)
    pl.semaphore_wait(barrier, len(peers))

    for e in range(1, wide):
        go(always, w_x(wsrc.at[q], q, p, lax.rem(p + e, wide)))
    for d in range(1, QUADS):
        for way in range(2):
            to = q + d if way == 0 else q - d
            live = to < QUADS if way == 0 else to >= 0
            go(live, w_z(q, lax.rem(to + QUADS, QUADS)))
    for k in range(pieces):
        go(q < last, tok_z(q, k, 0, lax.rem(q + 1, QUADS)))
        go(q > 0, tok_z(q, k, 1, lax.rem(q + last, QUADS)))
    own_w = pltpu.make_async_copy(wsrc.at[q], wall.at[:, :, owned(here)], own_s.at[0])
    own_w.start()

    def beyond(s):
        more = ((s < q) & (q < last)) | ((s > q) & (q > 0))
        return more, lax.rem(jnp.where(s < q, q + 1, q + last), QUADS)

    def relay(i, k):
        s = seqs[i]
        more, onward = beyond(s)
        tok_z(s, k, 0, q).wait_recv()
        go(more, tok_z(s, k, 0, onward))
        go(always, tok_t(s, k, j, 0, side))
        go(always, tok_t(s, k, j, 1, core))

    def relay_side(i, k):
        s = seqs[i]
        tok_t(s, k, flip(j, 2), 0, side).wait_recv()
        go(always, tok_t(s, k, flip(j, 2), 2, core))

    def arrive(i):
        s = seqs[i]
        for k in range(pieces):
            tok_t(s, k, flip(j, 1), 0, core).wait_recv()
            tok_t(s, k, flip(flip(j, 1), 2), 0, core).wait_recv()

    def forward(s):
        up_s, gate_s = par[q, :, 0:1], par[q, :, 1:2]
        tap = [par[q, :, 2 + k : 3 + k] for k in range(TAPS)]
        bias = par[q, :, 5:6]
        both = contract_last(wall[0:2].reshape(2 * deep, model), tok[0, s])
        up, gate = both[:deep] * up_s, both[deep:] * gate_s
        lane = lax.broadcasted_iota(jnp.int32, up.shape, 1)
        zero = jnp.zeros_like(up)
        late = [jnp.where(lane < TAPS - 1 - k, zero, pltpu.roll(up, TAPS - 1 - k, 1)) for k in range(TAPS - 1)] + [up]
        v = bias + tap[0] * late[0] + tap[1] * late[1] + tap[2] * late[2]
        square = v * v
        t = jnp.tanh(ROOT_2_PI * (v + CUBIC * (square * v)))
        rise = 0.5 * (1.0 + t)
        value = v * rise
        slope = rise + 0.5 * v * (1.0 - t * t) * (ROOT_2_PI * (1.0 + 3.0 * CUBIC * square))
        ct[2] = (value * gate).astype(ct.dtype)
        back = contract_last(wall[2], tok[1, s])
        ct[1] = (back * value * gate_s).astype(ct.dtype)
        conv_cot = back * gate * slope
        act_cot = tap[2] * conv_cot
        for k in range(TAPS - 1):
            early = pltpu.roll(conv_cot, tokens - (TAPS - 1 - k), 1)
            act_cot = act_cot + tap[k] * jnp.where(lane >= tokens - (TAPS - 1 - k), zero, early)
        ct[0] = (act_cot * up_s).astype(ct.dtype)
        sums = [jnp.sum(conv_cot * late[k], axis=1, keepdims=True) for k in range(TAPS)]
        sums.append(jnp.sum(conv_cot, axis=1, keepdims=True))
        for k, total in enumerate(sums):
            sm[0:deep, k : k + 1] = sm[0:deep, k : k + 1] + total

    def half_input(s, b):
        def block(i, carry):
            at = pl.ds(pl.multiple_of(b * 2 * width + i * BLOCK, BLOCK), BLOCK)
            total = contract_first(ct[0], wall[0, :, at]) + contract_first(ct[1], wall[1, :, at])
            gi[s, :, at] = total.astype(gi.dtype)
            return carry

        lax.fori_loop(0, 2 * width // BLOCK, block, 0)

    def input_grad(s):
        half_input(s, 1 - bit)
        go(always, c_copy(s))
        half_input(s, bit)

    def product(s, at):
        first = jnp.dot(ct[0:2].reshape(2 * deep, tokens), tok[0, s, :, at], preferred_element_type=jnp.float32)
        second = jnp.dot(ct[2], tok[1, s, :, at], preferred_element_type=jnp.float32)
        return first.reshape(2, deep, first.shape[-1]), second

    def weight_grad(s, fresh):
        def block(i, carry):
            at = pl.ds(pl.multiple_of(i * BLOCK, BLOCK), BLOCK)
            first, second = product(s, at)
            if fresh:
                acc[0:2, :, at] = first
                acc[2, :, at] = second
            else:
                acc[0:2, :, at] = acc[0:2, :, at] + first
                acc[2, :, at] = acc[2, :, at] + second
            return carry

        lax.fori_loop(0, model // BLOCK, block, 0)

    def close(s, fs):
        at = owned(fs)
        first, second = product(s, at)
        gw[0:2, :, at] = (acc[0:2, :, at] + first).astype(gw.dtype)
        gw[2, :, at] = (acc[2, :, at] + second).astype(gw.dtype)

    def core_sum(t):
        c_copy(t).wait_recv()

        def add(r):
            s1[t, r, :] = (f32(gi[t, r, halves(bit)]) + f32(rc[t, r, :])).astype(s1.dtype)

        rowwise(tokens, add)
        go(always, y_copy(t))

    def side_sum(t):
        y_copy(t).wait_recv()

        def add(r):
            s2[t, r, :] = (f32(s1[t, r, inner(half)]) + f32(ry[t, r, :])).astype(s2.dtype)

        rowwise(tokens, add)

    def chain(i):
        s = seqs[i]
        more, _ = beyond(s)
        onward = lax.rem(jnp.where(s < q, q + last, q + 1), QUADS)
        slot = jnp.where((onward == s) & (s < q), QUADS, s)

        @pl.when(more)
        def _():
            g_copy(s, s, q).wait_recv()

            def add(r):
                s2[s, r, :] = (f32(s2[s, r, :]) + f32(rz[s, r, :])).astype(s2.dtype)

            rowwise(tokens, add)

        go(always, g_copy(s, slot, onward))

    def send_grads(t):
        for e in range(1, wide):
            dst = lax.rem(p + e, wide)
            close(seqs[-1], t * wide + dst)
            go(always, x_copy(p, t, dst))
        close(seqs[-1], t * wide + p)

    def pass_grads(t, live):
        for e in range(1, wide):
            x_copy(lax.rem(p + e, wide), t, p).wait_recv()

        def add(i, carry):
            k, r = i // (deep // 8), pl.ds(pl.multiple_of(lax.rem(i, deep // 8) * 8, 8), 8)
            total = f32(gw[k, r, owned(t * wide + p)])
            for e in range(1, wide):
                total = total + f32(rx[lax.rem(p + e, wide), t, k, r, :])
            sw[t, k, r, :] = total.astype(sw.dtype)
            return carry

        for k in range(3):
            total = f32(gw[k, :, owned(t * wide + p)])
            for e in range(1, wide):
                total = total + f32(rx[lax.rem(p + e, wide), t, k])
            sw[t, k] = total.astype(sw.dtype)
        if live:
            go(always, z_copy(q, t))

    for i in range(1, QUADS):
        s = seqs[i]
        w_z(s, q).wait_recv()
        for e in range(1, wide):
            go(always, w_x(wall.at[:, :, owned(s * wide + p)], s, p, lax.rem(p + e, wide)))
    own_w.wait()
    for i in range(QUADS):
        for e in range(1, wide):
            w_x(wsrc.at[0], seqs[i], lax.rem(p + e, wide), p).wait_recv()

    for i in range(QUADS - 1):
        s = seqs[i]
        for k in range(CHUNKS):
            relay(i + 1, k)
        if i:
            arrive(i)
        forward(s)
        for k in range(CHUNKS, pieces):
            relay(i + 1, k)
        input_grad(s)
        for k in range(pieces):
            relay_side(i + 1, k)
        weight_grad(s, i == 0)
        if i:
            side_sum(seqs[i - 1])
        core_sum(s)
    s = seqs[-1]
    arrive(QUADS - 1)
    forward(s)
    input_grad(s)
    order = [seqs[3], seqs[2], seqs[1], seqs[0]]
    send_grads(order[0])
    core_sum(s)
    send_grads(order[1])
    side_sum(seqs[2])
    chain(2)
    send_grads(order[2])
    side_sum(seqs[3])
    chain(3)
    send_grads(order[3])
    flat = sm[...].T
    small[...] = flat[0 : small.shape[0], :]
    for d in range(1, n):
        go(always, m_copy(here, lax.rem(here + d, n)))
    own_m = pltpu.make_async_copy(small, smalls.at[here], own_s.at[1])
    own_m.start()
    pass_grads(order[0], True)
    pass_grads(order[1], True)
    chain(1)
    pass_grads(order[2], True)
    pass_grads(order[3], False)
    own_g = pltpu.make_async_copy(sw.at[q], wout.at[q], own_s.at[2])
    own_g.start()

    def seed(r):
        s3[r, :] = f32(s2[q, r, :])

    rowwise(tokens, seed)
    for live, slot in ((q > 0, q), (q < last, QUADS)):
        @pl.when(live)
        def _(slot=slot):
            g_copy(q, slot, q).wait_recv()

            def add(r):
                s3[r, :] = s3[r, :] + f32(rz[slot, r, :])

            rowwise(tokens, add)

    mine = quarter(width, j)

    def finish(r):
        gout[r, mine] = s3[r, :].astype(gout.dtype)

    rowwise(tokens, finish)
    go(always, t_copy(gout.at[:, mine], j, 0, side))
    go(always, t_copy(gout.at[:, mine], j, 1, core))
    t_copy(gout.at[:, mine], flip(j, 2), 0, side).wait_recv()
    go(always, t_copy(gout.at[:, quarter(width, flip(j, 2))], flip(j, 2), 2, core))
    t_copy(gout.at[:, mine], flip(j, 1), 0, core).wait_recv()
    t_copy(gout.at[:, mine], flip(flip(j, 1), 2), 0, core).wait_recv()
    for i in range(1, QUADS):
        z_copy(seqs[i], q).wait_recv()
    for d in range(1, n):
        m_copy(lax.rem(here + d, n), here).wait_recv()
    own_m.wait()
    own_g.wait()
    for live, copy in started:
        if live is always:
            copy.wait_send()
        else:
            @pl.when(live)
            def _():
                copy.wait_send()


def fused(
    n, n_tp,
    inputs,
    cotangent,
    up_weight,
    gate_weight,
    down_weight,
    up_scale,
    gate_scale,
    down_scale,
    conv_weight,
    conv_bias,
):
    wide = n // QUADS
    rows, cols = up_weight.shape
    part = cols // QUADS
    deep = -(-part // 16) * 16
    tall = -(-deep // LANES) * LANES
    tokens, model = inputs.shape
    width = model // 4

    wsrc = jnp.stack([up_weight.T.astype(BF), gate_weight.T.astype(BF), down_weight.astype(BF)])
    wsrc = wsrc.reshape(3, QUADS, part, rows).transpose(1, 0, 2, 3)
    wsrc = jnp.pad(wsrc, ((0, 0), (0, 0), (0, deep - part), (0, 0)))
    par = jnp.concatenate([up_scale[None], gate_scale[None], conv_weight, conv_bias[None]], axis=0)
    par = par.reshape(TAPS + 3, QUADS, part).transpose(1, 2, 0)
    par = jnp.pad(par, ((0, 0), (0, deep - part), (0, LANES - TAPS - 3)))

    pieces = 2 * CHUNKS
    wout, gout, smalls = pl.pallas_call(
        functools.partial(fused_kernel, n),
        out_shape=(
            jax.ShapeDtypeStruct((QUADS, 3, deep, rows), BF),
            jax.ShapeDtypeStruct((tokens, model), BF),
            jax.ShapeDtypeStruct((n, 8, tall), jnp.float32),
        ),
        in_specs=[VM] * 5,
        out_specs=(VM, VM, VM),
        scratch_shapes=[
            pltpu.VMEM((2, QUADS, tokens, model), BF),
            pltpu.VMEM((3, deep, model), BF),
            pltpu.VMEM((3, deep, tokens), BF),
            pltpu.VMEM((QUADS, tokens, model), BF),
            pltpu.VMEM((3, deep, model), jnp.float32),
            pltpu.VMEM((3, deep, model), BF),
            pltpu.VMEM((wide, QUADS, 3, deep, rows), BF),
            pltpu.VMEM((QUADS, 3, deep, rows), BF),
            pltpu.VMEM((QUADS, tokens, 2 * width), BF),
            pltpu.VMEM((QUADS, tokens, 2 * width), BF),
            pltpu.VMEM((QUADS, tokens, width), BF),
            pltpu.VMEM((QUADS, tokens, width), BF),
            pltpu.VMEM((QUADS + 1, tokens, width), BF),
            pltpu.VMEM((tokens, width), jnp.float32),
            pltpu.VMEM((tall, LANES), jnp.float32),
            pltpu.VMEM((8, tall), jnp.float32),
            DMA((QUADS, 2, pieces)), DMA((QUADS, pieces)), DMA((QUADS, 3, pieces)), DMA((QUADS, 4, pieces)),
            DMA((QUADS,)), DMA((QUADS,)), DMA((QUADS, wide)), DMA((QUADS, wide)),
            DMA((QUADS,)), DMA((QUADS,)), DMA((QUADS,)), DMA((QUADS,)),
            DMA((QUADS,)), DMA((QUADS + 1,)), DMA((3,)), DMA((4,)),
            DMA((QUADS, wide)), DMA((QUADS, wide)), DMA((QUADS,)), DMA((QUADS,)),
            DMA((n,)), DMA((n,)), DMA((3,)),
        ],
        compiler_params=pltpu.CompilerParams(
            collective_id=2, has_side_effects=True, vmem_limit_bytes=60 * 2**20
        ),
    )(inputs, cotangent, down_scale[None], wsrc, par)

    if n_tp > 4:
        groups = [[g * 4 + k for g in range(n_tp // 4)] for k in range(4)]
        gout = lax.psum(gout, "tp", axis_index_groups=groups)
    stats = jnp.sum(smalls.reshape(QUADS, wide, 8, tall)[:, :, : TAPS + 1, :part], axis=1)
    stats = stats.transpose(1, 0, 2).reshape(TAPS + 1, cols)
    grads = wout[:, :, :part].transpose(1, 0, 2, 3).reshape(3, cols, rows).astype(jnp.float32)
    return (gout, grads[0].T, grads[1].T, grads[2], stats[:TAPS], stats[TAPS])


def on_device(n, n_tp, inputs, cotangent, up_weight, *rest):
    rows, cols = up_weight.shape
    part, (tokens, model) = cols // QUADS, inputs.shape
    even = rows % LANES == 0 and part % 8 == 0 and tokens % LANES == 0 and model % (4 * BLOCK) == 0
    plan = fused if even and n == 2 * QUADS else general
    return plan(n, n_tp, inputs, cotangent, up_weight, *rest)


def solution(mesh):
    in_specs = (
        P("fs", None),
        P("fs", None),
        P("fs", "tp"),
        P("fs", "tp"),
        P("tp", "fs"),
        P("tp"),
        P("tp"),
        P(),
        P(None, "tp"),
        P("tp"),
    )
    out_specs = (P("fs", None), P("fs", "tp"), P("fs", "tp"), P("tp", "fs"), P(None, "tp"), P("tp"))
    return jax.shard_map(
        functools.partial(on_device, mesh.shape["fs"], mesh.shape["tp"]),
        mesh=mesh, in_specs=in_specs, out_specs=out_specs, check_vma=False,
    )
```
